256 devices in a mesh: sp: 16 (over y, x), tp: 16 (over z, core).
Axes of the slice: x: 4, y: 4, z: 8, core: 2. Of those that a mesh axis runs over, the one named last changes fastest.
Arguments:
- query_rows: bfloat16 [65536, 1024], P('sp', 'tp'), may hold values from -6 to 6
- key_rows: bfloat16 [65536, 1024], P('sp', 'tp'), may hold values from -6 to 6
- value_rows: bfloat16 [65536, 1024], P('sp', 'tp'), may hold values from -6 to 6
- gate_rows: bfloat16 [65536, 1024], P('sp', 'tp'), may hold values from -6 to 6
- log_decay: float32 [16, 65536], P('tp', 'sp'), may hold values from -1 to 0
- residual: bfloat16 [65536, 2048], P(('sp', 'tp')), may hold values from -6 to 6
- head_gain: float32 [1024], P('tp'), may hold values from 0.1 to 1.9
- out_weight: bfloat16 [1024, 2048], P(None, 'tp'), may hold values from -0.1875 to 0.1875
- norm_gain: float32 [2048], replicated, may hold values from 0.1 to 1.9
- expert_ids: int32 [65536, 2], P(('sp', 'tp')), may hold values from 0 to 15, all different within a row; in each aligned block of 256 rows (0 to 255, 256 to 511, ...) at most 48 rows name the same one
- route_weights: float32 [65536, 2], P(('sp', 'tp')), may hold values from 0.2 to 1
- expert_gate: bfloat16 [2048, 16384], P(None, ('sp', 'tp')), may hold values from -0.125 to 0.125
- expert_up: bfloat16 [2048, 16384], P(None, ('sp', 'tp')), may hold values from -0.125 to 0.125
- expert_down: bfloat16 [2048, 16384], P(None, ('sp', 'tp')), may hold values from -0.1875 to 0.1875
- shared_gate: bfloat16 [2048, 512], replicated, may hold values from -0.125 to 0.125
- shared_up: bfloat16 [2048, 512], replicated, may hold values from -0.125 to 0.125
- shared_down: bfloat16 [2048, 512], replicated, may hold values from -0.25 to 0.25
Outputs:
- result: bfloat16 [65536, 2048], P(('sp', 'tp'))
The draws below stay inside these ranges and needn't reach their ends.
Inputs may be any that keep to these rules, and one draw needn't show every extreme that they name: `expert_ids`: each row names 2 different experts. Within the rows of one device (aligned blocks of 256 rows) no expert is named by more than 48 rows, and in some block an expert is named by exactly 48 rows.
All inputs are finite; a program needn't handle non-finite values.
Results may differ from the reference program's by a relative error of at most 0.0075.
Values may be sent and summed in bfloat16 or wider, within the bound.
No kernel may reach another device: no remote copies, remote signals or barrier semaphores. Data moves between devices by JAX's collectives and lax.ppermute only.
A program may use at most 128 MiB of HBM per device.

```python
import math
import jax
import jax.numpy as jnp
import numpy as np
from jax import lax

D = 2048
HEADS = 16
HEAD = 64
HW = 1024
FF = 1024
SH = 512
TOPK = 2
SPAN = 512
TOK_DEV = 256
TOKENS = 65536
SPECIALISTS = 16
CAP = 48


def draw_log_decay(key, part):
    streams = jax.random.split(key, 6)
    slow_share = 0.5
    sequence_ordinals = jnp.arange(TOKENS, dtype=jnp.int32)
    chance = jax.random.uniform(streams[0], (HEADS,))
    slow = chance < slow_share
    fast_rate = jnp.exp(jax.random.uniform(streams[1], (HEADS,), minval=jnp.log(1.0 / 100.0), maxval=jnp.log(1.0 / 30.0)))
    slow_rate = jnp.exp(jax.random.uniform(streams[2], (HEADS,), minval=jnp.log(0.1), maxval=jnp.log(0.8))) / TOKENS
    rate = jnp.where(slow, slow_rate, fast_rate)
    factor = jnp.exp(jax.random.uniform(streams[3], (16,), minval=jnp.log(0.25), maxval=0.0))
    individual_slot_factor = factor[sequence_ordinals * 16 // TOKENS]
    constant_shrinkage = -rate[:, None] * individual_slot_factor[None, :]
    shifted_locations = jax.random.randint(streams[4], (HEADS, 2), 0, TOKENS)
    stack_level = jax.random.uniform(streams[5], (HEADS, 2), minval=jnp.log(0.5), maxval=jnp.log(0.8))
    segment_bundles = jnp.sum(jnp.where(sequence_ordinals[None, None, :] == shifted_locations[:, :, None], stack_level[:, :, None], 0.0), axis=1)
    return (constant_shrinkage + segment_bundles).astype(jnp.float32)


def block_levels(stream_key, dims, cuts, low, largest):
    gain = 1.0
    for dim, parts in cuts:
        heights = jax.random.uniform(jax.random.fold_in(jax.random.fold_in(stream_key, 6), dim), (parts,), jnp.float32, low / len(cuts), largest / len(cuts))
        gain = gain * jnp.repeat(jnp.exp(heights), dims[dim] // parts).reshape((-1,) + (1,) * (len(dims) - 1 - dim))
    return gain


def deal_out(rng, own, number, rows, count, top, reach, lean):
    sequence = jax.random.permutation(rng, count)
    crowded, common = load_shares(count, rows * top, reach, lean, True), load_shares(count, rows * top, reach, lean, False)
    places = jnp.arange(count)

    def named(lengths, offset_by):
        used = int((lengths > 0).sum())
        fixed = max(1, used // 4)
        moved = fixed + (places - fixed + offset_by * (used - fixed)) % max(1, count - fixed)
        return jnp.zeros((count,), jnp.int32).at[sequence[jnp.where(places < fixed, places, moved)]].set(jnp.asarray(lengths, jnp.int32))

    lengths = jnp.where(number % 4 == 0, named(crowded, number // 4), named(common, number - number // 4 - 1))
    mixed = jax.random.permutation(jax.random.fold_in(own, 3), count)
    giver, sink = mixed[0:count // 2 * 2:2], mixed[1:count // 2 * 2:2]
    slack = jnp.minimum(lengths[giver] - 1, reach - lengths[sink]) // 2
    slack = jnp.where((giver == sequence[0]) | (sink == sequence[0]) | (lengths[sink] == 0), 0, jnp.maximum(slack, 0))
    moved = jax.random.randint(jax.random.fold_in(own, 4), (count // 2,), 0, 1 << 20) % (slack + 1)
    lengths = lengths.at[giver].add(-moved).at[sink].add(moved)
    labels = jnp.searchsorted(jnp.cumsum(lengths), jnp.arange(rows * top), side="right").astype(jnp.int32)
    table = labels.reshape(top, rows).T
    table = table[jax.random.permutation(jax.random.fold_in(own, 1), rows)]
    offset_by = jax.random.randint(jax.random.fold_in(own, 2), (rows, 1), 0, top)
    return jnp.take_along_axis(table, (jnp.arange(top)[None, :] + offset_by) % top, axis=1)


def load_shares(number_of, total, reach, slope, full):
    portions = [(1 << 20) // math.isqrt(standing ** slope) + 1 for standing in range(1, number_of + 1)]
    largest = reach if full else min(reach, max(-(-total // number_of), total * portions[0] // sum(portions)))
    least = 1 if total - largest >= number_of - 1 else 0
    counts, rest = [largest] + [least] * (number_of - 1), total - largest - least * (number_of - 1)
    while rest > 0:
        candidates = [i for i in range(1, number_of) if counts[i] < largest] or [i for i in range(1, number_of) if counts[i] < reach]
        whole, budget = sum([portions[i] for i in candidates]), rest
        for i in candidates:
            addition = min(reach - counts[i], max(1, budget * portions[i] // whole), rest)
            counts[i] = counts[i] + addition
            rest = rest - addition
    return np.array(counts)


def centred(key, dims, scale, limit, pieces=(), kind=jnp.bfloat16):
    loudness = block_levels(key, dims, pieces, -0.22, 0.18) if pieces else 1.0
    array = jax.random.normal(key, dims, jnp.float32) * scale * loudness
    return jnp.minimum(jnp.maximum(array, -limit), limit).astype(kind)


def setup_inputs(seed: int = 0) -> dict:
    streams_of = jax.random.split(jax.random.key(seed), 18)
    query_rows = centred(streams_of[0], (TOKENS, HW), 1.0, 6.0, ((0, 16), (1, 16)))
    key_rows = centred(streams_of[1], (TOKENS, HW), 1.0, 6.0, ((0, 16), (1, 16)))
    value_rows = centred(streams_of[2], (TOKENS, HW), 1.0, 6.0, ((0, 16), (1, 16)))
    gate_rows = centred(streams_of[3], (TOKENS, HW), 1.0, 6.0, ((0, 16), (1, 16)))
    log_decay = draw_log_decay(jax.random.fold_in(streams_of[17], 71), 0)
    residual = centred(streams_of[5], (TOKENS, D), 1.0, 6.0, ((0, 256),))
    head_gain = jnp.clip(1.0 + 0.18 * jax.random.normal(streams_of[6], (HW,), jnp.float32), 0.1, 1.9)
    out_weight = centred(streams_of[7], (HW, D), HW ** -0.5, 0.1875, ((1, 16),))
    norm_gain = jnp.clip(1.0 + 0.18 * jax.random.normal(streams_of[8], (D,), jnp.float32), 0.1, 1.9)
    expert_ids_keys = jax.random.split(jax.random.fold_in(streams_of[9], 1), TOKENS // TOK_DEV)
    expert_ids_turns = jax.random.permutation(jax.random.fold_in(streams_of[9], 3), TOKENS // TOK_DEV)
    expert_ids = jax.vmap(lambda own, number: deal_out(jax.random.fold_in(streams_of[9], 2), own, number, TOK_DEV, SPECIALISTS, TOPK, CAP, 2))(expert_ids_keys, expert_ids_turns).reshape((TOKENS, TOPK))
    route_weights = jnp.clip(jnp.exp(math.log(1.0) - 1.609438 * jax.random.uniform(streams_of[10], (TOKENS, TOPK), jnp.float32) ** block_levels(streams_of[10], (TOKENS, TOPK), ((0, 256),), -0.2, 0.2)), 0.2, 1.0)
    expert_gate = centred(streams_of[11], (D, SPECIALISTS * FF), D ** -0.5, 0.125, ((1, 256),))
    expert_up = centred(streams_of[12], (D, SPECIALISTS * FF), D ** -0.5, 0.125, ((1, 256),))
    expert_down = centred(streams_of[13], (D, SPECIALISTS * FF), FF ** -0.5, 0.1875, ((1, 256),))
    shared_gate = centred(streams_of[14], (D, SH), D ** -0.5, 0.125)
    shared_up = centred(streams_of[15], (D, SH), D ** -0.5, 0.125)
    shared_down = centred(streams_of[16], (D, SH), SH ** -0.5, 0.25)
    return dict(query_rows=query_rows, key_rows=key_rows, value_rows=value_rows, gate_rows=gate_rows, log_decay=log_decay, residual=residual, head_gain=head_gain, out_weight=out_weight, norm_gain=norm_gain, expert_ids=expert_ids, route_weights=route_weights, expert_gate=expert_gate, expert_up=expert_up, expert_down=expert_down, shared_gate=shared_gate, shared_up=shared_up, shared_down=shared_down)


eps = 1e-05

def retain(queries, key_heads, values, log_decay):
    rows, heads, width = queries.shape
    count = rows // SPAN
    scale = width ** (-0.5)
    query_blocks = queries.reshape(count, SPAN, heads, width)
    key_blocks = key_heads.reshape(count, SPAN, heads, width)
    value_blocks = values.reshape(count, SPAN, heads, width)
    decay_blocks = log_decay.reshape(heads, count, SPAN).transpose(1, 0, 2)
    offsets = jnp.arange(SPAN, dtype=jnp.int32)
    causal = offsets[:, None] >= offsets[None, :]

    def advance(carry, inputs):
        block_queries, block_keys, block_values, decay_block = inputs
        query_matrix_full = block_queries.astype(jnp.float32)
        key_matrix_full = block_keys.astype(jnp.float32)
        value_matrix_full = block_values.astype(jnp.float32)
        running = jnp.cumsum(decay_block, axis=1)
        spread = running[:, :, None] - running[:, None, :]
        damping = jnp.exp(jnp.where(causal[None], spread, -jnp.inf))
        attention_scores = jnp.einsum('xru,jru->rxj', query_matrix_full, key_matrix_full)
        decay_weighted = lax.optimization_barrier((attention_scores * scale * damping).astype(jnp.bfloat16)).astype(jnp.float32)
        inner_block_term = jnp.einsum('svc,csj->vsj', decay_weighted, value_matrix_full)
        carried = jnp.einsum('nhd,hde->nhe', query_matrix_full, carry, precision=lax.Precision.HIGHEST)
        carried = carried * jnp.exp(running).T[:, :, None]
        decay_to_block_end = jnp.exp(running[:, -1:] - running).T[:, :, None] * scale
        state_update = jnp.einsum('jok,jow->okw', key_matrix_full * decay_to_block_end, value_matrix_full, precision=lax.Precision.HIGHEST)
        carry = carry * jnp.exp(running[:, -1])[:, None, None] + state_update
        return (carry, inner_block_term + carried)
    start = jnp.zeros((heads, width, width), jnp.float32)
    _, outputs = lax.scan(advance, start, (query_blocks, key_blocks, value_blocks, decay_blocks))
    return outputs.reshape(rows, heads, width)

def reference(query_rows, key_rows, value_rows, gate_rows, log_decay, residual, head_gain, out_weight, norm_gain, expert_ids, route_weights, expert_gate, expert_up, expert_down, shared_gate, shared_up, shared_down):
    retained = retain(query_rows.reshape(TOKENS, HEADS, HEAD), key_rows.reshape(TOKENS, HEADS, HEAD), value_rows.reshape(TOKENS, HEADS, HEAD), log_decay)
    centered = retained - lax.optimization_barrier(jnp.mean(retained, axis=2, keepdims=True))
    normed = centered * lax.rsqrt(lax.optimization_barrier(jnp.mean(centered * centered, axis=2, keepdims=True)) + eps)
    ret_rows = (normed.reshape(TOKENS, HW) * head_gain * jax.nn.silu(gate_rows.astype(jnp.float32))).astype(jnp.bfloat16)
    mixer = jnp.dot(ret_rows, out_weight, preferred_element_type=jnp.float32)
    hidden = (residual.astype(jnp.float32) + mixer).astype(jnp.bfloat16)
    hidden_wide = hidden.astype(jnp.float32)
    normed_rows = (hidden_wide * lax.rsqrt(lax.optimization_barrier(jnp.mean(hidden_wide * hidden_wide, axis=1, keepdims=True)) + eps) * norm_gain).astype(jnp.bfloat16)
    shared_mid = (jax.nn.silu(jnp.dot(normed_rows, shared_gate, preferred_element_type=jnp.float32)) * jnp.dot(normed_rows, shared_up, preferred_element_type=jnp.float32)).astype(jnp.bfloat16)
    shared_out = lax.dot_general(shared_mid, shared_down, (((1,), (1,)), ((), ())), preferred_element_type=jnp.float32)
    block_count = TOKENS // TOK_DEV
    slots = block_count * CAP
    block_index = jnp.arange(block_count, dtype=jnp.int32)[:, None]
    token_index = jnp.arange(TOKENS, dtype=jnp.int32)

    def expert_step(total, index):
        chosen = expert_ids == index
        picked = jnp.any(chosen, axis=1)
        weight = lax.optimization_barrier(jnp.sum(jnp.where(chosen, route_weights, 0.0), axis=1))
        blocked = picked.reshape(block_count, TOK_DEV).astype(jnp.int32)
        position = jnp.cumsum(blocked, axis=1) - 1
        target = jnp.where(blocked > 0, block_index * CAP + position, slots).reshape(-1).astype(jnp.int32)
        table = jnp.zeros((slots + 1,), jnp.int32).at[target].set(token_index)[:slots]
        live = jnp.zeros((slots + 1,), jnp.float32).at[target].set(1.0)[:slots]
        rows = normed_rows[table]
        gate_cols = lax.dynamic_slice_in_dim(expert_gate, index * FF, FF, 1)
        up_cols = lax.dynamic_slice_in_dim(expert_up, index * FF, FF, 1)
        down_cols = lax.dynamic_slice_in_dim(expert_down, index * FF, FF, 1)
        middle = (jax.nn.silu(jnp.dot(rows, gate_cols, preferred_element_type=jnp.float32)) * jnp.dot(rows, up_cols, preferred_element_type=jnp.float32)).astype(jnp.bfloat16)
        outcome = lax.dot_general(middle, down_cols, (((1,), (1,)), ((), ())), preferred_element_type=jnp.float32).astype(jnp.bfloat16)
        contrib = outcome.astype(jnp.float32) * (weight[table] * live)[:, None]
        return (total.at[table].add(contrib), None)
    routed, _ = lax.scan(expert_step, jnp.zeros((TOKENS, D), jnp.float32), jnp.arange(SPECIALISTS, dtype=jnp.int32))
    return (hidden_wide + routed + shared_out).astype(jnp.bfloat16)
```

```python
import functools

import jax
import jax.numpy as jnp
from jax import lax
from jax.experimental import pallas as pl
from jax.experimental.pallas import tpu as pltpu
from jax.sharding import PartitionSpec as P

HEAD = 64
SPAN = 512
EPS = 1e-05
SCALE = HEAD ** (-0.5)
CHUNKS = 2

f32 = jnp.float32
bf16 = jnp.bfloat16


def split3(x):
    hi = x.astype(bf16)
    rest = x - hi.astype(f32)
    mid = rest.astype(bf16)
    return hi, mid, (rest - mid.astype(f32)).astype(bf16)


def dot(a, b, dims):
    return lax.dot_general(a, b, (dims, ((), ())), preferred_element_type=f32)


def running_sum(x):
    lane = lax.broadcasted_iota(jnp.int32, x.shape, 1)
    shift = 1
    while shift < x.shape[1]:
        x = x + jnp.where(lane >= shift, pltpu.roll(x, shift, 1), 0.0)
        shift *= 2
    return x


def state_kernel(decay_ref, k_ref, v_ref, packed_ref, prefix_ref, run_ref):
    count = decay_ref.shape[1] // SPAN
    run = running_sum(
        jnp.concatenate(
            [decay_ref[:, b * SPAN : (b + 1) * SPAN] for b in range(count)], axis=0
        )
    )
    run_ref[...] = run
    ends = run[:, SPAN - 1 :]
    weight = jnp.exp(ends - run) * SCALE
    state = jnp.zeros((HEAD, HEAD), f32)
    total = jnp.zeros((1, 1), f32)
    for b in range(count):
        prefix_ref[b] = state
        cols = slice(b * SPAN, (b + 1) * SPAN)
        scaled = k_ref[:, cols].astype(f32) * weight[b : b + 1]
        vals = v_ref[:, cols]
        update = sum(dot(vals, part, ((1,), (1,))) for part in split3(scaled))
        state = state * jnp.exp(ends[b : b + 1]) + update
        total = total + ends[b : b + 1]
    half = HEAD // 2
    packed_ref[0:half, :] = jnp.concatenate([state[:half], state[half:]], axis=1)
    packed_ref[half:, :] = jnp.broadcast_to(jnp.exp(total), (8, 2 * HEAD))


def inner_kernel(run_ref, q_ref, k_ref, v_ref, out_ref):
    count = run_ref.shape[0]
    run = run_ref[...]
    run_cols = run.T
    part = SPAN // 2
    for b in range(count):
        base = b * SPAN
        keys = k_ref[:, base : base + SPAN].T
        for j in range(2):
            depth = (j + 1) * part
            scores = dot(
                keys[:depth],
                q_ref[:, base + j * part : base + depth],
                ((1,), (0,)),
            )
            spread = (
                run[b : b + 1, j * part : depth] - run_cols[:depth, b : b + 1]
            )
            earlier = lax.broadcasted_iota(jnp.int32, (depth, part), 0)
            later = lax.broadcasted_iota(jnp.int32, (depth, part), 1) + j * part
            damping = jnp.exp(jnp.where(earlier <= later, spread, -jnp.inf))
            weighted = (scores * SCALE * damping).astype(bf16)
            out_ref[:, base + j * part : base + depth] = dot(
                v_ref[:, base : base + depth], weighted, ((1,), (0,))
            )


def finish_kernel(
    place_ref, all_ref, prefix_ref, run_ref, inner_ref, q_ref, g_ref, gain_ref, out_ref
):
    place = place_ref[0]
    half = HEAD // 2
    packed = jnp.zeros((half, 2 * HEAD), f32)
    for i in range(all_ref.shape[0]):
        joined = packed * all_ref[i, half : half + 1, :] + all_ref[i, :half, :]
        packed = jnp.where(i < place, joined, packed)
    incoming = jnp.concatenate([packed[:, :HEAD], packed[:, HEAD:]], axis=0)
    run = run_ref[...]
    grow = jnp.exp(run)
    ends = run[:, SPAN - 1 :]
    row = lax.broadcasted_iota(jnp.int32, (HEAD, HEAD), 0)
    col = lax.broadcasted_iota(jnp.int32, (HEAD, HEAD), 1)
    gain = jnp.sum(
        jnp.where(row == col, jnp.broadcast_to(gain_ref[...], (HEAD, HEAD)), 0.0),
        axis=1,
        keepdims=True,
    )
    base = jnp.zeros((1, 1), f32)
    part = out_ref.shape[2]
    for b in range(run.shape[0]):
        cols = slice(b * SPAN, (b + 1) * SPAN)
        entering = prefix_ref[b] + jnp.exp(base) * incoming
        queries = q_ref[:, cols]
        carried = sum(dot(piece, queries, ((1,), (0,))) for piece in split3(entering))
        retained = inner_ref[:, cols] + carried * grow[b : b + 1]
        centered = retained - jnp.mean(retained, axis=0, keepdims=True)
        spread = jnp.mean(centered * centered, axis=0, keepdims=True)
        gate = g_ref[:, cols].astype(f32)
        rows = (
            centered * lax.rsqrt(spread + EPS) * gain * (gate * jax.nn.sigmoid(gate))
        ).astype(bf16)
        for i in range(SPAN // part):
            out_ref[b * (SPAN // part) + i] = rows[:, i * part : (i + 1) * part]
        base = base + ends[b : b + 1]


def mix_kernel(x_ref, w_ref, res_ref, gain_ref, slot_ref, hidden_ref, normed_ref, *outs):
    tokens, width = res_ref.shape
    cut = 2 * w_ref.shape[2]
    x = x_ref[...].T
    squares = jnp.zeros((tokens, 1), f32)
    for p in range(width // cut):
        cols = slice(p * cut, (p + 1) * cut)
        weight = jnp.concatenate([w_ref[2 * p], w_ref[2 * p + 1]], axis=1)
        mixed = dot(x, weight, ((1,), (0,)))
        hidden = (res_ref[:, cols].astype(f32) + mixed).astype(bf16)
        hidden_ref[:, cols] = hidden
        wide = hidden.astype(f32)
        squares = squares + jnp.sum(wide * wide, axis=1, keepdims=True)
    scale = lax.rsqrt(squares * (1.0 / width) + EPS)
    picks = []
    for c, out_ref in enumerate(outs):
        rows = out_ref.shape[0]
        index = lax.broadcasted_iota(jnp.int32, (rows, tokens), 0) + c * rows
        hit = (index == slot_ref[0:1, :]) | (index == slot_ref[1:2, :])
        picks.append(jnp.where(hit, 1.0, 0.0).astype(bf16))
    for p in range(width // cut):
        cols = slice(p * cut, (p + 1) * cut)
        normed = (
            hidden_ref[:, cols].astype(f32) * scale * gain_ref[:, cols]
        ).astype(bf16)
        normed_ref[:, cols] = normed
        for pick, out_ref in zip(picks, outs):
            out_ref[:, cols] = dot(pick, normed, ((1,), (0,))).astype(bf16)


def call(kernel, outs, args, flops, name, smem=()):
    def full(place):
        return pl.BlockSpec(memory_space=pltpu.SMEM if place in smem else pltpu.VMEM)

    moved = sum(a.size * a.dtype.itemsize for a in (*args, *outs))
    return pl.pallas_call(
        kernel,
        out_shape=outs,
        in_specs=[full(k) for k in range(len(args))],
        out_specs=[pl.BlockSpec(memory_space=pltpu.VMEM) for _ in outs],
        cost_estimate=pl.CostEstimate(flops=flops, bytes_accessed=moved, transcendentals=0),
        compiler_params=pltpu.CompilerParams(vmem_limit_bytes=48 * 1024 * 1024),
        name=name,
    )(*args)


def on_device(
    query_rows,
    key_rows,
    value_rows,
    gate_rows,
    log_decay,
    residual,
    head_gain,
    out_weight,
    norm_gain,
    expert_ids,
    route_weights,
    expert_gate,
    expert_up,
    expert_down,
    shared_gate,
    shared_up,
    shared_down,
):
    shape = jax.ShapeDtypeStruct
    seq_rows, local_width = query_rows.shape
    tokens, width = residual.shape
    experts = lax.axis_size("sp")
    columns = lax.axis_size("tp")
    blocks = seq_rows // SPAN
    out_full = lax.all_gather(out_weight, "tp", axis=0, tiled=False)
    gate_full = lax.all_gather(expert_gate.T, "tp", axis=0, tiled=True)
    up_full = lax.all_gather(expert_up.T, "tp", axis=0, tiled=True)
    down_full = lax.all_gather(expert_down.T, "tp", axis=0, tiled=True)

    queries, keys, values, gates = (a.T for a in (query_rows, key_rows, value_rows, gate_rows))
    packed, prefix, run = call(
        state_kernel,
        [
            shape((HEAD // 2 + 8, 2 * HEAD), f32),
            shape((blocks, HEAD, HEAD), f32),
            shape((blocks, SPAN), f32),
        ],
        [log_decay, keys, values],
        6 * seq_rows * HEAD * HEAD,
        "states",
    )
    everyone = lax.all_to_all(
        jnp.broadcast_to(packed[None], (experts, *packed.shape)), "sp", 0, 0, tiled=True
    )
    (inner,) = call(
        inner_kernel,
        [shape((HEAD, seq_rows), f32)],
        [run, queries, keys, values],
        4 * seq_rows * HEAD * SPAN,
        "inner",
    )
    place = lax.axis_index("sp").astype(jnp.int32).reshape(1)
    (ret_rows,) = call(
        finish_kernel,
        [shape((columns, HEAD, seq_rows // columns), bf16)],
        [place, everyone, prefix, run, inner, queries, gates, head_gain.reshape(1, -1)],
        6 * seq_rows * HEAD * HEAD,
        "finish",
        smem=(0,),
    )
    token_rows = lax.all_to_all(ret_rows, "tp", 0, 0, tiled=True)

    capacity = 3 * tokens * 2 // (2 * experts)
    share = capacity // CHUNKS
    ids = expert_ids.T
    each = jnp.arange(experts, dtype=jnp.int32)[:, None]
    named = [each == ids[j : j + 1] for j in range(2)]
    member = (named[0] | named[1]).astype(bf16)
    before = jnp.triu(jnp.ones((tokens, tokens), bf16), 1)
    position = jnp.dot(member, before, preferred_element_type=f32).astype(jnp.int32)
    spot = (position // share) * (experts * share) + each * share + position % share
    slots = jnp.stack([jnp.sum(jnp.where(n, spot, 0), axis=0) for n in named])

    rows = experts * share
    hidden, normed, *outgoing = call(
        mix_kernel,
        [shape((tokens, width), bf16)] * 2 + [shape((rows, width), bf16)] * CHUNKS,
        [
            token_rows.reshape(columns * HEAD, tokens),
            out_full,
            residual,
            norm_gain.reshape(1, -1),
            slots,
        ],
        2 * tokens * width * (columns * HEAD + rows * CHUNKS),
        "mix",
    )
    routing = route_weights.T
    routed = None
    for c in range(CHUNKS):
        arrived = lax.all_to_all(
            outgoing[c].reshape(experts, share, width), "sp", 0, 0, tiled=True
        ).reshape(rows, width)
        middle = (
            jax.nn.silu(dot(arrived, gate_full, ((1,), (1,))))
            * dot(arrived, up_full, ((1,), (1,)))
        ).astype(bf16)
        outcome = dot(middle, down_full, ((1,), (0,))).astype(bf16)
        returned = lax.all_to_all(
            outcome.reshape(experts, share, width), "sp", 0, 0, tiled=True
        ).reshape(rows, width)
        index = jnp.arange(rows, dtype=jnp.int32)[:, None] + c * rows
        spread = sum(
            jnp.where(index == slots[j : j + 1], routing[j : j + 1], 0.0) for j in range(2)
        )
        high = spread.astype(bf16)
        low = (spread - high.astype(f32)).astype(bf16)
        for piece in (high, low):
            term = dot(piece, returned, ((0,), (0,)))
            routed = term if routed is None else routed + term
    shared_mid = (
        jax.nn.silu(dot(normed, shared_gate, ((1,), (0,))))
        * dot(normed, shared_up, ((1,), (0,)))
    ).astype(bf16)
    shared_out = dot(shared_mid, shared_down, ((1,), (1,)))
    return (hidden.astype(f32) + routed + shared_out).astype(bf16)


def solution(mesh):
    placed = (
        P("sp", "tp"),
        P("sp", "tp"),
        P("sp", "tp"),
        P("sp", "tp"),
        P("tp", "sp"),
        P(("sp", "tp"), None),
        P("tp"),
        P(None, "tp"),
        P(),
        P(("sp", "tp"), None),
        P(("sp", "tp"), None),
        P(None, ("sp", "tp")),
        P(None, ("sp", "tp")),
        P(None, ("sp", "tp")),
        P(),
        P(),
        P(),
    )
    return jax.shard_map(
        on_device, mesh=mesh, in_specs=placed, out_specs=P(("sp", "tp"), None), check_vma=False
    )
```

```python
import functools

import jax
import jax.numpy as jnp
from jax import lax
from jax.experimental import pallas as pl
from jax.experimental.pallas import tpu as pltpu
from jax.sharding import PartitionSpec as P

HEAD = 64
SPAN = 512
EPS = 1e-05
SCALE = HEAD ** (-0.5)

f32 = jnp.float32
bf16 = jnp.bfloat16


def split3(x):
    hi = x.astype(bf16)
    rest = x - hi.astype(f32)
    mid = rest.astype(bf16)
    return hi, mid, (rest - mid.astype(f32)).astype(bf16)


def dot(a, b, dims):
    return lax.dot_general(a, b, (dims, ((), ())), preferred_element_type=f32)


def running_sum(x):
    lane = lax.broadcasted_iota(jnp.int32, x.shape, 1)
    shift = 1
    while shift < x.shape[1]:
        x = x + jnp.where(lane >= shift, pltpu.roll(x, shift, 1), 0.0)
        shift *= 2
    return x


def state_kernel(decay_ref, k_ref, v_ref, packed_ref, prefix_ref, run_ref):
    count = decay_ref.shape[1] // SPAN
    run = running_sum(
        jnp.concatenate(
            [decay_ref[:, b * SPAN : (b + 1) * SPAN] for b in range(count)], axis=0
        )
    )
    run_ref[...] = run
    ends = run[:, SPAN - 1 :]
    weight = jnp.exp(ends - run) * SCALE
    state = jnp.zeros((HEAD, HEAD), f32)
    total = jnp.zeros((1, 1), f32)
    for b in range(count):
        prefix_ref[b] = state
        cols = slice(b * SPAN, (b + 1) * SPAN)
        scaled = k_ref[:, cols].astype(f32) * weight[b : b + 1]
        vals = v_ref[:, cols]
        update = sum(dot(vals, part, ((1,), (1,))) for part in split3(scaled))
        state = state * jnp.exp(ends[b : b + 1]) + update
        total = total + ends[b : b + 1]
    half = HEAD // 2
    joined = jnp.concatenate([state[:half], state[half:]], axis=1)
    whole = jnp.broadcast_to(jnp.exp(total), (8, 2 * HEAD))
    for i in range(packed_ref.shape[0]):
        packed_ref[i, 0:half, :] = joined
        packed_ref[i, half:, :] = whole


def inner_kernel(run_ref, q_ref, k_ref, v_ref, out_ref):
    count = run_ref.shape[0]
    run = run_ref[...]
    run_cols = run.T
    part = SPAN // 2
    for b in range(count):
        base = b * SPAN
        keys = k_ref[:, base : base + SPAN].T
        for j in range(2):
            depth = (j + 1) * part
            scores = dot(
                keys[:depth],
                q_ref[:, base + j * part : base + depth],
                ((1,), (0,)),
            )
            spread = (
                run[b : b + 1, j * part : depth] - run_cols[:depth, b : b + 1]
            )
            earlier = lax.broadcasted_iota(jnp.int32, (depth, part), 0)
            later = lax.broadcasted_iota(jnp.int32, (depth, part), 1) + j * part
            damping = jnp.exp(jnp.where(earlier <= later, spread, -jnp.inf))
            weighted = (scores * SCALE * damping).astype(bf16)
            out_ref[:, base + j * part : base + depth] = dot(
                v_ref[:, base : base + depth], weighted, ((1,), (0,))
            )


def finish_kernel(
    place_ref, all_ref, prefix_ref, run_ref, inner_ref, q_ref, g_ref, gain_ref, out_ref
):
    place = place_ref[0]
    half = HEAD // 2
    packed = jnp.zeros((half, 2 * HEAD), f32)
    for i in range(all_ref.shape[0]):
        joined = packed * all_ref[i, half : half + 1, :] + all_ref[i, :half, :]
        packed = jnp.where(i < place, joined, packed)
    incoming = jnp.concatenate([packed[:, :HEAD], packed[:, HEAD:]], axis=0)
    run = run_ref[...]
    grow = jnp.exp(run)
    ends = run[:, SPAN - 1 :]
    row = lax.broadcasted_iota(jnp.int32, (HEAD, HEAD), 0)
    col = lax.broadcasted_iota(jnp.int32, (HEAD, HEAD), 1)
    gain = jnp.sum(
        jnp.where(row == col, jnp.broadcast_to(gain_ref[...], (HEAD, HEAD)), 0.0),
        axis=1,
        keepdims=True,
    )
    base = jnp.zeros((1, 1), f32)
    part = out_ref.shape[2]
    for b in range(run.shape[0]):
        cols = slice(b * SPAN, (b + 1) * SPAN)
        entering = prefix_ref[b] + jnp.exp(base) * incoming
        queries = q_ref[:, cols]
        carried = sum(dot(piece, queries, ((1,), (0,))) for piece in split3(entering))
        retained = inner_ref[:, cols] + carried * grow[b : b + 1]
        centered = retained - jnp.mean(retained, axis=0, keepdims=True)
        spread = jnp.mean(centered * centered, axis=0, keepdims=True)
        gate = g_ref[:, cols].astype(f32)
        rows = (
            centered * lax.rsqrt(spread + EPS) * gain * (gate * jax.nn.sigmoid(gate))
        ).astype(bf16)
        for i in range(SPAN // part):
            out_ref[b * (SPAN // part) + i] = rows[:, i * part : (i + 1) * part]
        base = base + ends[b : b + 1]


def held(refs):
    return refs[0][...] if len(refs) == 1 else jnp.concatenate([r[...] for r in refs], axis=0)


def mix_kernel(sizes, steps, place_ref, x_ref, res_ref, gain_ref, slot_ref, *refs):
    mine, theirs, refs = take(refs, sizes)
    hidden_ref, normed_ref, out_ref = refs
    tokens, width = res_ref.shape
    chips = len(sizes)
    cut = width // chips
    half = cut // 2
    chip, core = place_ref[0] // 2, lax.rem(place_ref[0], 2)
    x = x_ref[...].T
    squares = jnp.zeros((tokens, 1), f32)
    for k in range(chips):
        weight = jnp.concatenate([held(mine[k]), held(theirs[k])], axis=1)
        mixed = dot(x, weight, ((1,), (0,)))
        first = lax.rem(chip + steps[k] % chips, chips) * cut
        for i, side in enumerate((core, 1 - core)):
            start = pl.multiple_of(first + side * half, half)
            cols = pl.ds(start, half)
            hidden = (
                res_ref[:, cols].astype(f32) + mixed[:, i * half : (i + 1) * half]
            ).astype(bf16)
            hidden_ref[:, cols] = hidden
            wide = hidden.astype(f32)
            squares = squares + jnp.sum(wide * wide, axis=1, keepdims=True)
    scale = lax.rsqrt(squares * (1.0 / width) + EPS)
    rows = out_ref.shape[0]
    index = lax.broadcasted_iota(jnp.int32, (rows, tokens), 0)
    hit = (index == slot_ref[0:1, :]) | (index == slot_ref[1:2, :])
    pick = jnp.where(hit, 1.0, 0.0).astype(bf16)
    for p in range(chips):
        cols = slice(p * cut, (p + 1) * cut)
        normed = (
            hidden_ref[:, cols].astype(f32) * scale * gain_ref[:, cols]
        ).astype(bf16)
        normed_ref[:, cols] = normed
        out_ref[:, cols] = dot(pick, normed, ((1,), (0,))).astype(bf16)


def take(refs, sizes):
    lists, at = [], 0
    for _ in range(2):
        found = []
        for n in sizes:
            found.append(refs[at : at + n])
            at += n
        lists.append(found)
    return (*lists, refs[at:])


def expert_kernel(sizes, x_ref, *refs):
    mine, theirs, refs = take(refs, sizes)
    out_ref, gate_buf, up_buf, down_buf, mid_ref, sem = refs
    bufs = (gate_buf, up_buf, down_buf)
    part = gate_buf.shape[0] // (2 * len(sizes))
    cut = 256
    copies = [[] for _ in range(gate_buf.shape[0] // cut)]
    count = 0
    for at, refs_of in enumerate(shard for pair in zip(mine, theirs) for shard in pair):
        row = 0
        for ref in refs_of:
            done = 0
            while done < ref.shape[0]:
                which, inside = divmod(row, part)
                n = min(part - inside, ref.shape[0] - done)
                copies[at * part // cut].append(
                    pltpu.make_async_copy(
                        ref.at[pl.ds(done, n)],
                        bufs[which].at[pl.ds(at * part + inside, n)],
                        sem.at[count],
                    )
                )
                count += 1
                done += n
                row += n
    for group in copies:
        for copy in group:
            copy.start()
    rows, width = x_ref.shape
    block = min(rows, 256)
    for g, group in enumerate(copies):
        for copy in group:
            copy.wait()
        cols = slice(g * cut, (g + 1) * cut)

        def step(i, _, cols=cols):
            at = pl.ds(pl.multiple_of(i * block, block), block)
            x = x_ref[at, :]
            gate = dot(x, gate_buf[cols, :], ((1,), (1,)))
            up = dot(x, up_buf[cols, :], ((1,), (1,)))
            mid_ref[at, cols] = (gate * jax.nn.sigmoid(gate) * up).astype(bf16)
            return 0

        lax.fori_loop(0, rows // block, step, 0)

    def finish(n, _):
        cols = pl.ds(pl.multiple_of(n * cut, cut), cut)
        out_ref[:, cols] = dot(mid_ref[...], down_buf[:, cols], ((1,), (0,))).astype(bf16)
        return 0

    lax.fori_loop(0, width // cut, finish, 0)


def combine_kernel(base_ref, slot_ref, weight_ref, rows_ref, out_ref):
    tokens, width = base_ref.shape
    index = lax.broadcasted_iota(jnp.int32, (rows_ref.shape[0], tokens), 0)
    spread = sum(
        jnp.where(index == slot_ref[j : j + 1, :], weight_ref[j : j + 1, :], 0.0)
        for j in range(2)
    )
    high = spread.astype(bf16)
    low = (spread - high.astype(f32)).astype(bf16)
    both = jnp.concatenate([high.T, low.T], axis=0)
    cut = 256
    for n in range(width // cut):
        cols = slice(n * cut, (n + 1) * cut)
        routed = dot(both, rows_ref[:, cols], ((1,), (0,)))
        out_ref[:, cols] = (
            base_ref[:, cols] + routed[:tokens] + routed[tokens:]
        ).astype(bf16)


def around(value, shift):
    length = lax.axis_size("tp")
    return lax.ppermute(value, "tp", [(i, (i + shift) % length) for i in range(length)])


def swapped(value):
    length = lax.axis_size("tp")
    return lax.ppermute(value, "tp", [(i, i ^ 1) for i in range(length)])


def exchanged(value, axis):
    return lax.all_to_all(value, axis, 0, 0, tiled=True)


def call(kernel, outs, args, flops, smem=(), hbm=(), scratch=(), limit=None):
    def full(place):
        space = pltpu.SMEM if place in smem else pltpu.HBM if place in hbm else pltpu.VMEM
        return pl.BlockSpec(memory_space=space)

    moved = sum(a.size * a.dtype.itemsize for a in (*args, *outs))
    return pl.pallas_call(
        kernel,
        out_shape=outs,
        in_specs=[full(k) for k in range(len(args))],
        out_specs=[pl.BlockSpec(memory_space=pltpu.VMEM) for _ in outs],
        cost_estimate=pl.CostEstimate(flops=flops, bytes_accessed=moved, transcendentals=0),
        scratch_shapes=scratch,
        compiler_params=pltpu.CompilerParams(vmem_limit_bytes=limit),
    )(*args)


def on_device(
    query_rows,
    key_rows,
    value_rows,
    gate_rows,
    log_decay,
    residual,
    head_gain,
    out_weight,
    norm_gain,
    expert_ids,
    route_weights,
    expert_gate,
    expert_up,
    expert_down,
    shared_gate,
    shared_up,
    shared_down,
):
    shape = jax.ShapeDtypeStruct
    seq_rows, _ = query_rows.shape
    tokens, width = residual.shape
    experts = lax.axis_size("sp")
    columns = lax.axis_size("tp")
    blocks = seq_rows // SPAN
    chips = columns // 2
    part = expert_gate.shape[1]
    first = jnp.concatenate([expert_gate.T, expert_up.T[: part // 2]], axis=0)
    second = jnp.concatenate([expert_up.T[part // 2 :], expert_down.T], axis=0)

    queries, keys, values, gates = (a.T for a in (query_rows, key_rows, value_rows, gate_rows))
    packed, prefix, run = call(
        state_kernel,
        [
            shape((experts, HEAD // 2 + 8, 2 * HEAD), f32),
            shape((blocks, HEAD, HEAD), f32),
            shape((blocks, SPAN), f32),
        ],
        [log_decay, keys, values],
        6 * seq_rows * HEAD * HEAD,
    )
    everyone = exchanged(packed, "sp")
    (inner,) = call(
        inner_kernel,
        [shape((HEAD, seq_rows), f32)],
        [run, queries, keys, values],
        4 * seq_rows * HEAD * SPAN,
    )
    place = lax.axis_index("sp").astype(jnp.int32).reshape(1)
    (ret_rows,) = call(
        finish_kernel,
        [shape((columns, HEAD, seq_rows // columns), bf16)],
        [place, everyone, prefix, run, inner, queries, gates, head_gain.reshape(1, -1)],
        6 * seq_rows * HEAD * HEAD,
        smem=(0,),
    )
    token_rows = exchanged(ret_rows, "tp")

    capacity = 3 * tokens * 2 // (2 * experts)
    ids = expert_ids.T
    each = jnp.arange(experts, dtype=jnp.int32)[:, None]
    named = [each == ids[j : j + 1] for j in range(2)]
    member = (named[0] | named[1]).astype(bf16)
    before = jnp.triu(jnp.ones((tokens, tokens), bf16), 1)
    position = jnp.dot(member, before, preferred_element_type=f32).astype(jnp.int32)
    spot = each * capacity + position
    slots = jnp.stack([jnp.sum(jnp.where(n, spot, 0), axis=0) for n in named])

    def chain(own, shift, hops):
        found = [own]
        for _ in range(1, hops + 1):
            found.append(around(found[-1], shift))
        return found

    def both(shards):
        return [(k, held_by, tuple(swapped(a) for a in held_by)) for k, held_by in shards]

    far = chips // 2
    mixing = both(
        [
            (-k if sign > 0 else k, (a,))
            for sign, hops in ((1, far), (-1, far - 1))
            for k, a in enumerate(chain(out_weight, 2 * sign, hops))
            if k or sign > 0
        ]
    )
    rows = experts * capacity
    mine = [a for _, held_by, _ in mixing for a in held_by]
    theirs = [a for _, _, held_by in mixing for a in held_by]
    sizes = [len(held_by) for _, held_by, _ in mixing]
    hidden, normed, outgoing = call(
        functools.partial(mix_kernel, sizes, [k for k, _, _ in mixing]),
        [shape((tokens, width), bf16)] * 2 + [shape((rows, width), bf16)],
        [
            lax.axis_index("tp").astype(jnp.int32).reshape(1),
            token_rows.reshape(columns * HEAD, tokens),
            residual,
            norm_gain.reshape(1, -1),
            slots,
            *mine,
            *theirs,
        ],
        2 * tokens * width * (columns * HEAD + rows),
        smem=(0,),
        limit=32 * 1024 * 1024,
    )

    first_on, first_back = chain(first, 2, far), chain(first, -2, far - 1)
    second_on, second_back = chain(second, 2, far - 1), chain(second, -2, far)
    routes = [(0, (first, second))]
    for k in range(1, far):
        routes += [(-k, (first_on[k], second_on[k])), (k, (first_back[k], second_back[k]))]
    routes = both([*routes, (far, (first_on[far], second_back[far]))])
    arrived = exchanged(outgoing.reshape(experts, capacity, width), "sp").reshape(rows, width)
    mine = [a for _, held_by, _ in routes for a in held_by]
    theirs = [a for _, _, held_by in routes for a in held_by]
    hidden_units = columns * part
    (outcome,) = call(
        functools.partial(expert_kernel, [len(held_by) for _, held_by, _ in routes]),
        [shape((rows, width), bf16)],
        [arrived, *mine, *theirs],
        6 * rows * width * hidden_units,
        hbm=tuple(range(1, 1 + len(mine) + len(theirs))),
        scratch=[pltpu.VMEM((hidden_units, width), bf16)] * 3
        + [
            pltpu.VMEM((rows, hidden_units), bf16),
            pltpu.SemaphoreType.DMA((8 * len(routes),)),
        ],
        limit=32 * 1024 * 1024,
    )
    returned = exchanged(outcome.reshape(experts, capacity, width), "sp").reshape(rows, width)
    shared_mid = (
        jax.nn.silu(dot(normed, shared_gate, ((1,), (0,))))
        * dot(normed, shared_up, ((1,), (0,)))
    ).astype(bf16)
    shared_out = dot(shared_mid, shared_down, ((1,), (1,)))
    (result,) = call(
        combine_kernel,
        [shape((tokens, width), bf16)],
        [hidden.astype(f32) + shared_out, slots, route_weights.T, returned],
        4 * rows * tokens * width,
    )
    return result


def solution(mesh):
    placed = (
        P("sp", "tp"),
        P("sp", "tp"),
        P("sp", "tp"),
        P("sp", "tp"),
        P("tp", "sp"),
        P(("sp", "tp"), None),
        P("tp"),
        P(None, "tp"),
        P(),
        P(("sp", "tp"), None),
        P(("sp", "tp"), None),
        P(None, ("sp", "tp")),
        P(None, ("sp", "tp")),
        P(None, ("sp", "tp")),
        P(),
        P(),
        P(),
    )
    return jax.shard_map(
        on_device, mesh=mesh, in_specs=placed, out_specs=P(("sp", "tp"), None), check_vma=False
    )
```
